32 devices in a mesh: gr: 2 (over x), sp: 8 (over z, y), tp: 2 (over core).
Axes of the slice: x: 2, y: 2, z: 4, core: 2. Of those that a mesh axis runs over, the one named last changes fastest.
Arguments:
- prompt_block_input: bfloat16 [16, 2048, 2048], P('gr', 'sp'), may hold values from -6 to 6
- key_projection_weight: bfloat16 [2048, 512], P(None, 'tp'), may hold values from -0.125 to 0.125
- value_projection_weight: bfloat16 [2048, 512], P(None, 'tp'), may hold values from -0.125 to 0.125
- forget_gate_weight: bfloat16 [8, 2048], P('tp'), may hold values from -0.125 to 0.125
- forget_gate_bias: float32 [8], P('tp'), may hold values from 3.5 to 12
- forget_gate_scale: float32 [16, 8, 2048], P('gr', 'tp', 'sp'), may hold values from 0.15 to 6
- gate_spike_added: float32 [16, 8, 2048], P('gr', 'tp', 'sp'), may hold values from -0.7 to 0
- prior_key_value_cache: bfloat16 [16, 14336, 8, 128], P(('gr', 'sp'), None, 'tp')
- prior_cumulative_log_forget: float32 [16, 8, 14336], P(('gr', 'sp'), 'tp'), as said below
- decoded_token_query: bfloat16 [16, 1024], P('gr', 'tp')
- decoded_token_key: bfloat16 [16, 512], P(('gr', 'sp'), 'tp'), may hold values from -6 to 6
- decoded_token_value: bfloat16 [16, 512], P(('gr', 'sp'), 'tp'), may hold values from -6 to 6
- decoded_log_gate: float32 [16, 8], P(('gr', 'sp'), 'tp'), may hold values from -2.5 to -0.05
- key_norm_gain: float32 [64], replicated, may hold values from 0.1 to 1.9
- read_norm_gain: float32 [1024], P('tp'), may hold values from 0.1 to 1.9
Outputs:
- new_cache: bfloat16 [16, 2048, 8, 128], P(('gr', 'sp'), None, 'tp')
- new_logc: float32 [16, 8, 2048], P(('gr', 'sp'), 'tp')
- next_read: bfloat16 [16, 1024], P(('gr', 'sp'), 'tp')
The draws below stay inside these ranges and needn't reach their ends.
Inputs may be any that keep to these rules, and one draw needn't show every extreme that they name: `prior_cumulative_log_forget`: each position's cumulative log forget value from the start of its sequence.
All inputs are finite; a program needn't handle non-finite values.
Results may differ from the reference program's by a relative error of at most 0.008.
Values may be sent and summed in bfloat16 or wider, within the bound.
A program may use at most 128 MiB of HBM per device.

```python
import jax
import jax.numpy as jnp
from jax import lax

D = 2048
HEADS = 16
KEY_VALUE_HEADS = 8
HEAD_DIM = 64
LENGTH = 16384
BLOCK_POSITIONS = 2048
PAST_POSITIONS = 14336
KV_WIDTH = 512
SPAN = 256
SEQUENCE_COUNT = 16


def head_speeds(key):
    picks = jax.random.randint(jax.random.fold_in(key, 40), (KEY_VALUE_HEADS,), 0, 8)
    return picks < 4


def spike_field(key, sequence_length):
    spike_positions = jax.random.randint(jax.random.fold_in(key, 1), (SEQUENCE_COUNT, 4), 0, sequence_length)
    spike_marks = jnp.any(jnp.arange(sequence_length)[None, None, :] == spike_positions[:, :, None], axis=1)
    spike_depth = jax.random.uniform(jax.random.fold_in(key, 2), (SEQUENCE_COUNT, KEY_VALUE_HEADS, sequence_length), jnp.float32, -0.7, -0.22)
    return jnp.where(spike_marks[:, None, :], spike_depth, 0.0)


def draw_forget_gate_bias(key, part):
    fast_heads = head_speeds(key)
    reach_span = jax.random.uniform(jax.random.fold_in(key, 45), (KEY_VALUE_HEADS,), jnp.float32, 30.0, 100.0)
    chain_total = jax.random.uniform(jax.random.fold_in(key, 46), (KEY_VALUE_HEADS,), jnp.float32, 0.8, 2.0)
    slow_bias = jnp.log(1.65 * float(LENGTH) / chain_total)
    return jnp.where(fast_heads, jnp.log(1.65 * reach_span), slow_bias)


def draw_forget_gate_scale(key, part):
    blocks = BLOCK_POSITIONS // SPAN
    block_index = (jnp.arange(BLOCK_POSITIONS) // SPAN).astype(jnp.float32)
    ramp_slope = jnp.log(3.0)
    ramp_log = ramp_slope * (block_index / max(blocks - 1, 1) - 0.5)
    block_level = jax.random.uniform(jax.random.fold_in(key, 50), (SEQUENCE_COUNT, 1, blocks), jnp.float32, -0.35, 0.35)
    block_level = jnp.repeat(block_level, SPAN, axis=-1)
    random_noise = jax.random.uniform(jax.random.fold_in(key, 51), (SEQUENCE_COUNT, KEY_VALUE_HEADS, BLOCK_POSITIONS), jnp.float32, -0.3, 0.3)
    return jnp.exp(ramp_log[None, None, :] + block_level + random_noise)


def draw_gate_spike_added(key, part):
    return spike_field(jax.random.fold_in(key, 60), BLOCK_POSITIONS)


def draw_prior_cumulative_log_forget(key, part):
    fast_heads = head_speeds(key)
    reach_span = jax.random.uniform(jax.random.fold_in(key, 47), (KEY_VALUE_HEADS,), jnp.float32, 30.0, 100.0)
    chain_total = jax.random.uniform(jax.random.fold_in(key, 48), (KEY_VALUE_HEADS,), jnp.float32, 0.8, 2.0)
    decay_step_rate = jnp.where(fast_heads, 1.0 / reach_span, chain_total / float(LENGTH))
    sequence_factor = jnp.exp(jax.random.uniform(jax.random.fold_in(key, 43), (SEQUENCE_COUNT, 1, 1), jnp.float32, -0.7, 0.7))
    random_noise = jnp.exp(jax.random.uniform(jax.random.fold_in(key, 44), (SEQUENCE_COUNT, KEY_VALUE_HEADS, PAST_POSITIONS), jnp.float32, -0.5, 0.5))
    log_forget_value = -decay_step_rate[None, :, None] * sequence_factor * random_noise + spike_field(jax.random.fold_in(key, 49), PAST_POSITIONS)
    return jnp.cumsum(log_forget_value, axis=-1)


def draw_prior_key_value_cache(key, part):
    drawn = jax.random.normal(jax.random.fold_in(key, 20), (SEQUENCE_COUNT, PAST_POSITIONS, KEY_VALUE_HEADS, HEAD_DIM), jnp.float32)
    key_part = drawn.astype(jnp.bfloat16)
    value_part = jax.random.normal(jax.random.fold_in(key, 24), (SEQUENCE_COUNT, PAST_POSITIONS, KEY_VALUE_HEADS, HEAD_DIM), jnp.float32)
    value_part = jnp.clip(value_part, -6.0, 6.0).astype(jnp.bfloat16)
    return jnp.concatenate([key_part, value_part], axis=-1)


def draw_decoded_token_query(key, part):
    drawn = jax.random.normal(jax.random.fold_in(key, 30), (SEQUENCE_COUNT, HEADS, HEAD_DIM), jnp.float32)
    return drawn.reshape(SEQUENCE_COUNT, HEADS * HEAD_DIM).astype(jnp.bfloat16)


def steps_of(own_key, dims, cuts, least, top_value):
    factor_of, own = 1.0, jax.random.fold_in(own_key, 6)
    for axis_at, blocks in cuts:
        heights = jnp.exp(jax.random.uniform(jax.random.fold_in(own, axis_at), (blocks,), jnp.float32, least / len(cuts), top_value / len(cuts)))
        factor_of = factor_of * jnp.repeat(heights, dims[axis_at] // blocks).reshape([-1 if axis == axis_at else 1 for axis in range(len(dims))])
    return factor_of


def scatter_about(own_key, dims, scale, most, shards=(), dtype=jnp.bfloat16):
    entries = scale * jax.random.normal(own_key, dims, jnp.float32)
    if shards:
        entries = entries * steps_of(own_key, dims, shards, -0.22, 0.18)
    return jnp.clip(entries, -most, most).astype(dtype)


def setup_inputs(seed: int = 0) -> dict:
    keys = jax.random.split(jax.random.key(seed), 16)
    return {
        "prompt_block_input": scatter_about(keys[0], (SEQUENCE_COUNT, BLOCK_POSITIONS, D), 1.0, 6.0, ((0, 2), (1, 8))),
        "key_projection_weight": scatter_about(keys[1], (D, KV_WIDTH), D ** -0.5, 0.125, ((1, 2),)),
        "value_projection_weight": scatter_about(keys[2], (D, KV_WIDTH), D ** -0.5, 0.125, ((1, 2),)),
        "forget_gate_weight": scatter_about(keys[3], (KEY_VALUE_HEADS, D), D ** -0.5, 0.125, ((0, 2),)),
        "forget_gate_bias": draw_forget_gate_bias(jax.random.fold_in(keys[15], 71), 0),
        "forget_gate_scale": draw_forget_gate_scale(jax.random.fold_in(keys[15], 71), 0),
        "gate_spike_added": draw_gate_spike_added(jax.random.fold_in(keys[15], 71), 0),
        "prior_key_value_cache": draw_prior_key_value_cache(jax.random.fold_in(keys[15], 71), 0),
        "prior_cumulative_log_forget": draw_prior_cumulative_log_forget(jax.random.fold_in(keys[15], 71), 0),
        "decoded_token_query": draw_decoded_token_query(jax.random.fold_in(keys[15], 71), 0),
        "decoded_token_key": scatter_about(keys[10], (SEQUENCE_COUNT, KV_WIDTH), 1.0, 6.0, ((0, 16), (1, 2))),
        "decoded_token_value": scatter_about(keys[11], (SEQUENCE_COUNT, KV_WIDTH), 1.0, 6.0, ((0, 16), (1, 2))),
        "decoded_log_gate": jnp.clip(-2.5 + 2.45 * jax.random.uniform(keys[12], (SEQUENCE_COUNT, KEY_VALUE_HEADS), jnp.float32) ** steps_of(keys[12], (SEQUENCE_COUNT, KEY_VALUE_HEADS), ((0, 16), (1, 2)), -0.2, 0.2), -2.5, -0.05),
        "key_norm_gain": jnp.clip(1.0 + 0.18 * jax.random.normal(keys[13], (HEAD_DIM,), jnp.float32), 0.1, 1.9),
        "read_norm_gain": jnp.clip(1.0 + 0.18 * jax.random.normal(keys[14], (HEADS * HEAD_DIM,), jnp.float32), 0.1, 1.9),
    }


EPSILON = 1e-06

def round_trip(weights):
    return lax.optimization_barrier(weights.astype(jnp.bfloat16)).astype(jnp.float32)

def reference(prompt_block_input, key_projection_weight, value_projection_weight, forget_gate_weight, forget_gate_bias, forget_gate_scale, gate_spike_added, prior_key_value_cache, prior_cumulative_log_forget, decoded_token_query, decoded_token_key, decoded_token_value, decoded_log_gate, key_norm_gain, read_norm_gain):
    seq_count = prompt_block_input.shape[0]
    group_size = HEADS // KEY_VALUE_HEADS
    flat_rows = prompt_block_input.reshape(seq_count * BLOCK_POSITIONS, D)
    key_raw = jnp.dot(flat_rows, key_projection_weight, preferred_element_type=jnp.float32)
    key_raw = key_raw.reshape(seq_count, BLOCK_POSITIONS, KEY_VALUE_HEADS, HEAD_DIM)
    normed = key_raw * lax.rsqrt(lax.optimization_barrier(jnp.mean(key_raw * key_raw, axis=-1, keepdims=True)) + EPSILON) * key_norm_gain
    block_keys = normed.astype(jnp.bfloat16)
    block_values = jnp.dot(flat_rows, value_projection_weight, preferred_element_type=jnp.float32)
    block_values = block_values.reshape(seq_count, BLOCK_POSITIONS, KEY_VALUE_HEADS, HEAD_DIM).astype(jnp.bfloat16)
    new_cache = jnp.concatenate([block_keys, block_values], axis=-1)
    gate_preactivation = jnp.einsum('spd,hd->shp', prompt_block_input.astype(jnp.float32), forget_gate_weight.astype(jnp.float32))
    gate_preactivation = gate_preactivation + forget_gate_bias[None, :, None]
    log_forget_value = forget_gate_scale * jax.nn.log_sigmoid(gate_preactivation) + gate_spike_added
    new_logc = prior_cumulative_log_forget[:, :, -1:] + jnp.cumsum(log_forget_value, axis=-1)
    final_logc = new_logc[:, :, -1] + decoded_log_gate
    scale = HEAD_DIM ** (-0.5)

    def read_one(items):
        query, rows_past, logc_past, rows_block, logc_block, key_own, value_own, final_one = items
        query_heads = query.astype(jnp.float32).reshape(KEY_VALUE_HEADS, group_size, HEAD_DIM)
        rows_all = jnp.concatenate([rows_past, rows_block], axis=0).astype(jnp.float32)
        keys_all = rows_all[:, :, :HEAD_DIM]
        values_all = rows_all[:, :, HEAD_DIM:]
        logc_all = jnp.concatenate([logc_past, logc_block], axis=1)
        scores = jnp.einsum('kge,lke->kgl', query_heads, keys_all) * scale
        scores = scores + final_one[:, None, None] - logc_all[:, None, :]
        own_heads = key_own.astype(jnp.float32).reshape(KEY_VALUE_HEADS, HEAD_DIM)
        own_score = jnp.einsum('kge,ke->kg', query_heads, own_heads) * scale
        row_top = jnp.maximum(lax.optimization_barrier(jnp.max(scores, axis=-1)), own_score)
        weights = round_trip(jnp.exp(scores - row_top[..., None]))
        own_weight = round_trip(jnp.exp(own_score - row_top))
        weighted = jnp.einsum('kgl,lke->kge', weights, values_all)
        weighted = weighted + own_weight[..., None] * value_own.astype(jnp.float32).reshape(KEY_VALUE_HEADS, 1, HEAD_DIM)
        normed_read = weighted * lax.rsqrt(lax.optimization_barrier(jnp.mean(weighted * weighted, axis=-1, keepdims=True)) + EPSILON)
        return (normed_read.reshape(HEADS * HEAD_DIM) * read_norm_gain).astype(jnp.bfloat16)
    next_read = lax.map(read_one, (decoded_token_query, prior_key_value_cache, prior_cumulative_log_forget, new_cache, new_logc, decoded_token_key, decoded_token_value, final_logc))
    return (new_cache, new_logc, next_read)
```

```python
import functools

import jax
import jax.numpy as jnp
from jax import lax
from jax.experimental import pallas as pl
from jax.experimental.pallas import tpu as pltpu
from jax.sharding import PartitionSpec as P

EPSILON = 1e-06
LOW = -1e30
MESH = pl.DeviceIdType.MESH
F32 = jnp.float32
BF16 = jnp.bfloat16


def step_pair(i, n):
    m = max(n // 2, 1)
    return 2 * ((m // 2 + m - i // 2) % m) + i % 2


def flip(me, k, n):
    if n & (n - 1):
        return (me + k) % n
    out = 0
    bit = 1
    while bit < n:
        a = (me // bit) % 2
        b = (k // bit) % 2
        out = out + bit * (a + b - 2 * a * b)
        bit *= 2
    return out


def back(me, k, n):
    if n & (n - 1):
        return (me + n - k) % n
    return flip(me, k, n)


def expander(positions, kv):
    shape = (positions, positions * kv)
    p = lax.broadcasted_iota(jnp.int32, shape, 0)
    r = lax.broadcasted_iota(jnp.int32, shape, 1)
    return jnp.where((r >= p * kv) & (r < p * kv + kv), 1.0, 0.0).astype(BF16)


def expand(values, matrix):
    rows = values.shape[0]
    high = values.astype(BF16).astype(F32)
    rest = values - high
    middle = rest.astype(BF16).astype(F32)
    low = rest - middle
    pieces = jnp.concatenate([high, middle, low], axis=0).astype(BF16)
    out = jnp.dot(pieces, matrix, preferred_element_type=F32)
    return out[:rows] + out[rows : 2 * rows] + out[2 * rows :]


def column(row):
    k = row.shape[1]
    eye = lax.broadcasted_iota(jnp.int32, (k, k), 0) == lax.broadcasted_iota(jnp.int32, (k, k), 1)
    return jnp.sum(jnp.where(eye, jnp.broadcast_to(row, (k, k)), 0.0), axis=1, keepdims=True)


def same_head(rows, count, kv):
    a = lax.broadcasted_iota(jnp.int32, (rows, count), 0)
    b = lax.broadcasted_iota(jnp.int32, (rows, count), 1)
    return lax.rem(a, kv) == lax.rem(b, kv)


def attend(query, keys, bias, scale, kv):
    s = lax.dot_general(query, keys, (((1,), (1,)), ((), ())), preferred_element_type=F32)
    s = s * scale + bias
    return jnp.where(same_head(s.shape[0], s.shape[1], kv), s, LOW)


def kernel(
    dims,
    x_hbm, wk_hbm, wv_hbm, wg_ref, bias_ref, scale_ref, spike_ref, cache_hbm, prior_hbm,
    query_ref, own_key_ref, own_value_ref, own_gate_ref, key_gain_ref, read_gain_ref,
    new_cache_hbm, new_logc_ref, read_ref,
    x_v, wk_v, wv_v, cache_v, prior_v, stage, send_v, recv_v, csend_v, crecv_v,
    expand_v, part_m, part_acc,
    x_sem, w_sem, cache_sem, prior_sem, send_sem, recv_sem, csend_sem, crecv_sem, out_sem,
):
    n, span, kv, head_dim, group, reps, chunk, sub = dims
    rows = reps * kv
    chunks = cache_sem.shape[0]
    chunk_rows = chunk * kv
    att_scale = head_dim ** (-0.5)
    me = lax.axis_index("sp")

    def x_copy(i):
        s = flip(me, step_pair(i, n), n)
        return pltpu.make_async_copy(x_hbm.at[s], x_v.at[s], x_sem.at[i])

    def cache_copy(c):
        at = pl.ds(pl.multiple_of(c * chunk_rows, chunk_rows), chunk_rows)
        return pltpu.make_async_copy(cache_hbm.at[at], cache_v.at[at], cache_sem.at[c])

    wk_copy = pltpu.make_async_copy(wk_hbm, wk_v, w_sem.at[0])
    wv_copy = pltpu.make_async_copy(wv_hbm, wv_v, w_sem.at[1])
    prior_copy = pltpu.make_async_copy(prior_hbm, prior_v, prior_sem)
    x_copy(0).start()
    wk_copy.start()
    wv_copy.start()

    @pl.loop(1, n)
    def _(i):
        x_copy(i).start()

    barrier = pltpu.get_barrier_semaphore()

    @pl.loop(1, n)
    def _(k):
        pl.semaphore_signal(barrier, inc=1, device_id={"sp": (me + k) % n}, device_id_type=MESH)

    prior_copy.start()

    @pl.loop(0, chunks)
    def _(c):
        cache_copy(c).start()

    expand_v[...] = expander(sub, kv)
    bias_col = column(bias_ref[...])
    own_gate_col = column(own_gate_ref[...])
    key_gain = key_gain_ref[...]
    upper = jnp.where(
        lax.broadcasted_iota(jnp.int32, (span, span), 0) <= lax.broadcasted_iota(jnp.int32, (span, span), 1),
        1.0, 0.0,
    )
    pl.semaphore_wait(barrier, n - 1)
    wk_copy.wait()
    wv_copy.wait()

    def remote(i, s):
        return (
            pltpu.make_async_remote_copy(
                src_ref=send_v.at[i], dst_ref=recv_v.at[me], send_sem=send_sem.at[i],
                recv_sem=recv_sem.at[me], device_id={"sp": s}, device_id_type=MESH,
            ),
            pltpu.make_async_remote_copy(
                src_ref=csend_v.at[i], dst_ref=crecv_v.at[me], send_sem=csend_sem.at[i],
                recv_sem=crecv_sem.at[me], device_id={"sp": s}, device_id_type=MESH,
            ),
        )

    @pl.loop(0, n)
    def _(i):
        k = step_pair(i, n)
        s = flip(me, k, n)
        x_copy(i).wait()
        xb = x_v[s]
        keys = jnp.dot(xb, wk_v[...], preferred_element_type=F32)
        values = jnp.dot(xb, wv_v[...], preferred_element_type=F32)
        for h in range(kv):
            kh = keys[:, h * head_dim : (h + 1) * head_dim]
            vh = values[:, h * head_dim : (h + 1) * head_dim]
            kh = kh * lax.rsqrt(jnp.mean(kh * kh, axis=-1, keepdims=True) + EPSILON) * key_gain
            row = jnp.concatenate([kh, vh], axis=-1)
            if kv == 1:
                stage[...] = row
            else:
                stage[pl.ds(h, span, stride=kv), :] = row
        send_v[i] = stage[...].astype(BF16)
        pre = lax.dot_general(
            wg_ref[...], xb, (((1,), (1,)), ((), ())), preferred_element_type=F32
        ) + bias_col
        log_sig = jnp.minimum(pre, 0.0) - jnp.log1p(jnp.exp(-jnp.abs(pre)))
        log_forget = scale_ref[s] * log_sig + spike_ref[s]
        csend_v[i] = jnp.dot(
            log_forget, upper, preferred_element_type=F32, precision=lax.Precision.HIGHEST
        )

        @pl.when(k != 0)
        def _():
            block, sums = remote(i, s)
            sums.start()
            block.start()

        @pl.when(k == 0)
        def _():
            pltpu.make_async_copy(send_v.at[i], recv_v.at[me], recv_sem.at[me]).start()
            pltpu.make_async_copy(csend_v.at[i], crecv_v.at[me], crecv_sem.at[me]).start()

    every = query_ref[...].astype(F32)
    own = lax.broadcasted_iota(jnp.int32, every.shape, 0) == me
    all_query = jnp.sum(jnp.where(own, every, 0.0), axis=0, keepdims=True)
    zeros = jnp.zeros((1, head_dim), F32)
    pieces = []
    for rep in range(reps):
        for h in range(kv):
            at = (h * group + rep % group) * head_dim
            pieces.append(jnp.concatenate([all_query[:, at : at + head_dim], zeros], axis=1))
    query = jnp.concatenate(pieces, axis=0)
    query_b = query.astype(BF16)

    prior_copy.wait()
    prior_last = prior_v[:, prior_v.shape[1] - 1 :]

    def repeat_rows(values):
        return jnp.concatenate([values] * reps, axis=0)

    def past_step(c, carry):
        top, acc = carry
        cache_copy(c).wait()
        keys = cache_v[pl.ds(pl.multiple_of(c * chunk_rows, chunk_rows), chunk_rows), :]
        distance = repeat_rows(prior_last - prior_v[:, pl.ds(pl.multiple_of(c * chunk, chunk), chunk)])
        bias = jnp.concatenate(
            [expand(distance[:, j * sub : (j + 1) * sub], expand_v[...]) for j in range(chunk // sub)], axis=1
        )
        s = attend(query_b, keys, bias, att_scale, kv)
        new_top = jnp.maximum(top, jnp.max(s, axis=1, keepdims=True))
        weights = jnp.exp(s - new_top).astype(BF16)
        acc = acc * jnp.exp(top - new_top) + jnp.dot(weights, keys, preferred_element_type=F32)
        return new_top, acc

    past_top, past_acc = lax.fori_loop(
        0, chunks, past_step,
        (jnp.full((rows, 1), LOW, F32), jnp.zeros((rows, 2 * head_dim), F32)),
    )

    block_expander = expander(span, kv)

    def out_copy(b):
        at = pl.ds(pl.multiple_of(b * span * kv, span * kv), span * kv)
        return pltpu.make_async_copy(recv_v.at[b], new_cache_hbm.at[at], out_sem.at[b])

    @pl.loop(0, n)
    def _(i):
        k = step_pair(i, n)
        b = back(me, k, n)

        @pl.when(k != 0)
        def _():
            pltpu.make_async_remote_copy(
                src_ref=csend_v.at[i], dst_ref=crecv_v.at[b], send_sem=csend_sem.at[i],
                recv_sem=crecv_sem.at[b], device_id={"sp": b}, device_id_type=MESH,
            ).wait_recv()
            pltpu.make_async_remote_copy(
                src_ref=send_v.at[i], dst_ref=recv_v.at[b], send_sem=send_sem.at[i],
                recv_sem=recv_sem.at[b], device_id={"sp": b}, device_id_type=MESH,
            ).wait_recv()

        @pl.when(k == 0)
        def _():
            pltpu.make_async_copy(csend_v.at[i], crecv_v.at[b], crecv_sem.at[b]).wait()
            pltpu.make_async_copy(send_v.at[i], recv_v.at[b], recv_sem.at[b]).wait()

        out_copy(b).start()
        keys = recv_v[b]
        bias = expand(repeat_rows(-crecv_v[b]), block_expander)
        s = attend(query_b, keys, bias, att_scale, kv)
        top = jnp.max(s, axis=1, keepdims=True)
        weights = jnp.exp(s - top).astype(BF16)
        part_m[b] = jnp.broadcast_to(top, (rows, 2 * head_dim))
        part_acc[b] = jnp.dot(weights, keys, preferred_element_type=F32)

    before = jnp.zeros((kv, 1), F32)
    tops = [past_top]
    accs = [past_acc]
    for b in range(n):
        sums = crecv_v[b]
        new_logc_ref[:, b * span : (b + 1) * span] = prior_last + before + sums
        tops.append(part_m[b][:, :1] - repeat_rows(before))
        accs.append(part_acc[b])
        before = before + sums[:, span - 1 :]
    final = repeat_rows(before + own_gate_col)

    own_key = own_key_ref[...].astype(F32)
    own_value = own_value_ref[...].astype(F32)
    own_keys = jnp.concatenate(
        [own_key[:, h * head_dim : (h + 1) * head_dim] for _ in range(reps) for h in range(kv)], axis=0
    )
    own_values = jnp.concatenate(
        [own_value[:, h * head_dim : (h + 1) * head_dim] for _ in range(reps) for h in range(kv)], axis=0
    )
    own_top = jnp.sum(query[:, :head_dim] * own_keys, axis=1, keepdims=True) * att_scale - final
    row_top = own_top
    for t in tops:
        row_top = jnp.maximum(row_top, t)
    total = jnp.zeros((rows, 2 * head_dim), F32)
    for t, a in zip(tops, accs):
        total = total + a * jnp.exp(t - row_top)
    own_weight = jnp.exp(own_top - row_top).astype(BF16).astype(F32)
    weighted = total[:, head_dim:] + own_weight * own_values
    normed = weighted * lax.rsqrt(jnp.mean(weighted * weighted, axis=1, keepdims=True) + EPSILON)
    flat = jnp.concatenate(
        [normed[g * kv + h : g * kv + h + 1, :] for h in range(kv) for g in range(group)], axis=1
    )
    read_ref[...] = (flat * read_gain_ref[...]).astype(BF16)

    @pl.loop(0, n)
    def _(i):
        k = step_pair(i, n)
        s = flip(me, k, n)
        out_copy(s).wait()

        @pl.when(k != 0)
        def _():
            block, sums = remote(i, s)
            sums.wait_send()
            block.wait_send()


def local(
    n,
    prompt_block_input,
    key_projection_weight,
    value_projection_weight,
    forget_gate_weight,
    forget_gate_bias,
    forget_gate_scale,
    gate_spike_added,
    prior_key_value_cache,
    prior_cumulative_log_forget,
    decoded_token_query,
    decoded_token_key,
    decoded_token_value,
    decoded_log_gate,
    key_norm_gain,
    read_norm_gain,
):
    head_dim = key_norm_gain.shape[0]
    _, past, kv, width = prior_key_value_cache.shape
    _, span, model = prompt_block_input.shape
    group = decoded_token_query.shape[1] // (kv * head_dim)
    reps = max(group, -(-8 // kv))
    rows = reps * kv
    sub = 256
    chunk = 1024
    while past % chunk:
        chunk //= 2
    sub = min(sub, chunk)
    chunks = past // chunk
    block_rows = span * kv
    vmem = pl.BlockSpec(memory_space=pltpu.VMEM)
    hbm = pl.BlockSpec(memory_space=pl.ANY)
    new_cache, new_logc, read = pl.pallas_call(
        functools.partial(kernel, (n, span, kv, head_dim, group, reps, chunk, sub)),
        out_shape=(
            jax.ShapeDtypeStruct((n * block_rows, width), BF16),
            jax.ShapeDtypeStruct((kv, n * span), F32),
            jax.ShapeDtypeStruct((1, group * kv * head_dim), BF16),
        ),
        in_specs=[hbm, hbm, hbm, vmem, vmem, vmem, vmem, hbm, hbm] + [vmem] * 6,
        out_specs=(hbm, vmem, vmem),
        scratch_shapes=[
            pltpu.VMEM((n, span, model), BF16),
            pltpu.VMEM((model, kv * head_dim), BF16),
            pltpu.VMEM((model, kv * head_dim), BF16),
            pltpu.VMEM((past * kv, width), BF16),
            pltpu.VMEM((kv, past), F32),
            pltpu.VMEM((block_rows, width), F32),
            pltpu.VMEM((n, block_rows, width), BF16),
            pltpu.VMEM((n, block_rows, width), BF16),
            pltpu.VMEM((n, kv, span), F32),
            pltpu.VMEM((n, kv, span), F32),
            pltpu.VMEM((sub, sub * kv), BF16),
            pltpu.VMEM((n, rows, width), F32),
            pltpu.VMEM((n, rows, width), F32),
            pltpu.SemaphoreType.DMA((n,)),
            pltpu.SemaphoreType.DMA((2,)),
            pltpu.SemaphoreType.DMA((chunks,)),
            pltpu.SemaphoreType.DMA,
            pltpu.SemaphoreType.DMA((n,)),
            pltpu.SemaphoreType.DMA((n,)),
            pltpu.SemaphoreType.DMA((n,)),
            pltpu.SemaphoreType.DMA((n,)),
            pltpu.SemaphoreType.DMA((n,)),
        ],
        compiler_params=pltpu.CompilerParams(
            collective_id=0, has_side_effects=True, vmem_limit_bytes=60 * 1024 * 1024
        ),
    )(
        prompt_block_input,
        key_projection_weight,
        value_projection_weight,
        forget_gate_weight,
        forget_gate_bias.reshape(1, -1),
        forget_gate_scale,
        gate_spike_added,
        prior_key_value_cache.reshape(past * kv, width),
        prior_cumulative_log_forget.reshape(kv, past),
        decoded_token_query,
        decoded_token_key,
        decoded_token_value,
        decoded_log_gate,
        key_norm_gain.reshape(1, -1),
        read_norm_gain.reshape(1, -1),
    )
    return (
        new_cache.reshape(1, n * span, kv, width),
        new_logc.reshape(1, kv, n * span),
        read,
    )


def solution(mesh):
    return jax.shard_map(
        functools.partial(local, mesh.shape["sp"]),
        mesh=mesh,
        in_specs=(
            P("gr", "sp", None),
            P(None, "tp"),
            P(None, "tp"),
            P("tp", None),
            P("tp"),
            P("gr", "tp", "sp"),
            P("gr", "tp", "sp"),
            P(("gr", "sp"), None, "tp", None),
            P(("gr", "sp"), "tp", None),
            P("gr", "tp"),
            P(("gr", "sp"), "tp"),
            P(("gr", "sp"), "tp"),
            P(("gr", "sp"), "tp"),
            P(),
            P("tp"),
        ),
        out_specs=(
            P(("gr", "sp"), None, "tp", None),
            P(("gr", "sp"), "tp", None),
            P(("gr", "sp"), "tp"),
        ),
        check_vma=False,
    )
```

```python
import functools

import jax
import jax.numpy as jnp
from jax import lax
from jax.experimental import pallas as pl
from jax.experimental.pallas import tpu as pltpu
from jax.sharding import PartitionSpec as P

EPSILON = 1e-06
LOW = -1e30
MESH = pl.DeviceIdType.MESH
F32 = jnp.float32
BF16 = jnp.bfloat16


def step_pair(i, n):
    m = max(n // 2, 1)
    return 2 * ((m // 2 + m - i // 2) % m) + i % 2


def flip(me, k, n):
    if n & (n - 1):
        return (me + k) % n
    out = 0
    bit = 1
    while bit < n:
        a = (me // bit) % 2
        b = (k // bit) % 2
        out = out + bit * (a + b - 2 * a * b)
        bit *= 2
    return out


def back(me, k, n):
    if n & (n - 1):
        return (me + n - k) % n
    return flip(me, k, n)


def expander(positions, kv):
    shape = (positions, positions * kv)
    p = lax.broadcasted_iota(jnp.int32, shape, 0)
    r = lax.broadcasted_iota(jnp.int32, shape, 1)
    return jnp.where((r >= p * kv) & (r < p * kv + kv), 1.0, 0.0).astype(BF16)


def expand(values, matrix):
    rows = values.shape[0]
    high = values.astype(BF16).astype(F32)
    rest = values - high
    middle = rest.astype(BF16).astype(F32)
    low = rest - middle
    pieces = jnp.concatenate([high, middle, low], axis=0).astype(BF16)
    out = jnp.dot(pieces, matrix, preferred_element_type=F32)
    return out[:rows] + out[rows : 2 * rows] + out[2 * rows :]


def column(row):
    k = row.shape[1]
    eye = lax.broadcasted_iota(jnp.int32, (k, k), 0) == lax.broadcasted_iota(jnp.int32, (k, k), 1)
    return jnp.sum(jnp.where(eye, jnp.broadcast_to(row, (k, k)), 0.0), axis=1, keepdims=True)


def same_head(rows, count, kv):
    a = lax.broadcasted_iota(jnp.int32, (rows, count), 0)
    b = lax.broadcasted_iota(jnp.int32, (rows, count), 1)
    return lax.rem(a, kv) == lax.rem(b, kv)


def attend(query, keys, bias, scale, kv):
    s = lax.dot_general(query, keys, (((1,), (1,)), ((), ())), preferred_element_type=F32)
    s = s * scale + bias
    return jnp.where(same_head(s.shape[0], s.shape[1], kv), s, LOW)


def kernel(
    dims,
    x_hbm, wk_hbm, wv_hbm, wg_ref, bias_ref, scale_ref, spike_ref, cache_hbm, prior_hbm,
    query_ref, own_key_ref, own_value_ref, own_gate_ref, key_gain_ref, read_gain_ref,
    recv_v, new_logc_ref, read_ref,
    x_v, wk_v, wv_v, cache_v, prior_v, stage, send_v, csend_v, crecv_v,
    expand_v, part_m, part_acc,
    x_sem, w_sem, cache_sem, prior_sem, send_sem, recv_sem, csend_sem, crecv_sem,
):
    n, span, kv, head_dim, group, reps, chunk, sub = dims
    rows = reps * kv
    chunks = cache_sem.shape[0]
    chunk_rows = chunk * kv
    att_scale = head_dim ** (-0.5)
    me = lax.axis_index("sp")

    def x_copy(i):
        s = flip(me, step_pair(i, n), n)
        return pltpu.make_async_copy(x_hbm.at[s], x_v.at[s], x_sem.at[i])

    def cache_copy(c):
        at = pl.ds(pl.multiple_of(c * chunk_rows, chunk_rows), chunk_rows)
        return pltpu.make_async_copy(cache_hbm.at[at], cache_v.at[at], cache_sem.at[c])

    wk_copy = pltpu.make_async_copy(wk_hbm, wk_v, w_sem.at[0])
    wv_copy = pltpu.make_async_copy(wv_hbm, wv_v, w_sem.at[1])
    prior_copy = pltpu.make_async_copy(prior_hbm, prior_v, prior_sem)
    x_copy(0).start()
    wk_copy.start()
    wv_copy.start()
    ahead = min(3, n)
    for i in range(1, ahead):
        x_copy(i).start()

    barrier = pltpu.get_barrier_semaphore()

    @pl.loop(1, n)
    def _(k):
        pl.semaphore_signal(barrier, inc=1, device_id={"sp": (me + k) % n}, device_id_type=MESH)

    expand_v[...] = expander(sub, kv)
    bias_col = column(bias_ref[...])
    own_gate_col = column(own_gate_ref[...])
    key_gain = key_gain_ref[...]
    upper = jnp.where(
        lax.broadcasted_iota(jnp.int32, (span, span), 0) <= lax.broadcasted_iota(jnp.int32, (span, span), 1),
        1.0, 0.0,
    )
    wk_copy.wait()
    wv_copy.wait()

    def remote(i, s):
        return (
            pltpu.make_async_remote_copy(
                src_ref=send_v.at[i], dst_ref=recv_v.at[me], send_sem=send_sem.at[i],
                recv_sem=recv_sem.at[me], device_id={"sp": s}, device_id_type=MESH,
            ),
            pltpu.make_async_remote_copy(
                src_ref=csend_v.at[i], dst_ref=crecv_v.at[me], send_sem=csend_sem.at[i],
                recv_sem=crecv_sem.at[me], device_id={"sp": s}, device_id_type=MESH,
            ),
        )

    @pl.loop(0, n)
    def _(i):
        k = step_pair(i, n)
        s = flip(me, k, n)
        x_copy(i).wait()

        @pl.when(i + ahead < n)
        def _():
            x_copy(i + ahead).start()

        @pl.when(i == n // 2)
        def _():
            prior_copy.start()

            @pl.loop(0, chunks)
            def _(c):
                cache_copy(c).start()

        xb = x_v[s]
        keys = jnp.dot(xb, wk_v[...], preferred_element_type=F32)
        values = jnp.dot(xb, wv_v[...], preferred_element_type=F32)
        for h in range(kv):
            kh = keys[:, h * head_dim : (h + 1) * head_dim]
            vh = values[:, h * head_dim : (h + 1) * head_dim]
            kh = kh * lax.rsqrt(jnp.mean(kh * kh, axis=-1, keepdims=True) + EPSILON) * key_gain
            row = jnp.concatenate([kh, vh], axis=-1)
            if kv == 1:
                stage[...] = row
            else:
                stage[pl.ds(h, span, stride=kv), :] = row
        send_v[i] = stage[...].astype(BF16)
        pre = lax.dot_general(
            wg_ref[...], xb, (((1,), (1,)), ((), ())), preferred_element_type=F32
        ) + bias_col
        log_sig = jnp.minimum(pre, 0.0) - jnp.log1p(jnp.exp(-jnp.abs(pre)))
        log_forget = scale_ref[s] * log_sig + spike_ref[s]
        csend_v[i] = jnp.dot(
            log_forget, upper, preferred_element_type=F32, precision=lax.Precision.HIGHEST
        )

        @pl.when(i == 0)
        def _():
            pl.semaphore_wait(barrier, n - 1)

        @pl.when(k != 0)
        def _():
            block, sums = remote(i, s)
            sums.start()
            block.start()

        @pl.when(k == 0)
        def _():
            pltpu.make_async_copy(send_v.at[i], recv_v.at[me], recv_sem.at[me]).start()
            pltpu.make_async_copy(csend_v.at[i], crecv_v.at[me], crecv_sem.at[me]).start()

    every = query_ref[...].astype(F32)
    own = lax.broadcasted_iota(jnp.int32, every.shape, 0) == me
    all_query = jnp.sum(jnp.where(own, every, 0.0), axis=0, keepdims=True)
    zeros = jnp.zeros((1, head_dim), F32)
    pieces = []
    for rep in range(reps):
        for h in range(kv):
            at = (h * group + rep % group) * head_dim
            pieces.append(jnp.concatenate([all_query[:, at : at + head_dim], zeros], axis=1))
    query = jnp.concatenate(pieces, axis=0)
    query_b = query.astype(BF16)

    prior_copy.wait()
    prior_last = prior_v[:, prior_v.shape[1] - 1 :]

    def repeat_rows(values):
        return jnp.concatenate([values] * reps, axis=0)

    def past_step(c, carry):
        top, acc = carry
        cache_copy(c).wait()
        keys = cache_v[pl.ds(pl.multiple_of(c * chunk_rows, chunk_rows), chunk_rows), :]
        distance = repeat_rows(prior_last - prior_v[:, pl.ds(pl.multiple_of(c * chunk, chunk), chunk)])
        bias = jnp.concatenate(
            [expand(distance[:, j * sub : (j + 1) * sub], expand_v[...]) for j in range(chunk // sub)], axis=1
        )
        s = attend(query_b, keys, bias, att_scale, kv)
        new_top = jnp.maximum(top, jnp.max(s, axis=1, keepdims=True))
        weights = jnp.exp(s - new_top).astype(BF16)
        acc = acc * jnp.exp(top - new_top) + jnp.dot(weights, keys, preferred_element_type=F32)
        return new_top, acc

    past_top, past_acc = lax.fori_loop(
        0, chunks, past_step,
        (jnp.full((rows, 1), LOW, F32), jnp.zeros((rows, 2 * head_dim), F32)),
    )

    block_expander = expander(span, kv)

    @pl.loop(0, n)
    def _(i):
        k = step_pair(i, n)
        b = back(me, k, n)

        @pl.when(k != 0)
        def _():
            pltpu.make_async_remote_copy(
                src_ref=csend_v.at[i], dst_ref=crecv_v.at[b], send_sem=csend_sem.at[i],
                recv_sem=crecv_sem.at[b], device_id={"sp": b}, device_id_type=MESH,
            ).wait_recv()
            pltpu.make_async_remote_copy(
                src_ref=send_v.at[i], dst_ref=recv_v.at[b], send_sem=send_sem.at[i],
                recv_sem=recv_sem.at[b], device_id={"sp": b}, device_id_type=MESH,
            ).wait_recv()

        @pl.when(k == 0)
        def _():
            pltpu.make_async_copy(csend_v.at[i], crecv_v.at[b], crecv_sem.at[b]).wait()
            pltpu.make_async_copy(send_v.at[i], recv_v.at[b], recv_sem.at[b]).wait()

        keys = recv_v[b]
        bias = expand(repeat_rows(-crecv_v[b]), block_expander)
        s = attend(query_b, keys, bias, att_scale, kv)
        top = jnp.max(s, axis=1, keepdims=True)
        weights = jnp.exp(s - top).astype(BF16)
        part_m[b] = jnp.broadcast_to(top, (rows, 2 * head_dim))
        part_acc[b] = jnp.dot(weights, keys, preferred_element_type=F32)

    before = jnp.zeros((kv, 1), F32)
    tops = [past_top]
    accs = [past_acc]
    for b in range(n):
        sums = crecv_v[b]
        new_logc_ref[:, b * span : (b + 1) * span] = prior_last + before + sums
        tops.append(part_m[b][:, :1] - repeat_rows(before))
        accs.append(part_acc[b])
        before = before + sums[:, span - 1 :]
    final = repeat_rows(before + own_gate_col)

    own_key = own_key_ref[...].astype(F32)
    own_value = own_value_ref[...].astype(F32)
    own_keys = jnp.concatenate(
        [own_key[:, h * head_dim : (h + 1) * head_dim] for _ in range(reps) for h in range(kv)], axis=0
    )
    own_values = jnp.concatenate(
        [own_value[:, h * head_dim : (h + 1) * head_dim] for _ in range(reps) for h in range(kv)], axis=0
    )
    own_top = jnp.sum(query[:, :head_dim] * own_keys, axis=1, keepdims=True) * att_scale - final
    row_top = own_top
    for t in tops:
        row_top = jnp.maximum(row_top, t)
    total = jnp.zeros((rows, 2 * head_dim), F32)
    for t, a in zip(tops, accs):
        total = total + a * jnp.exp(t - row_top)
    own_weight = jnp.exp(own_top - row_top).astype(BF16).astype(F32)
    weighted = total[:, head_dim:] + own_weight * own_values
    normed = weighted * lax.rsqrt(jnp.mean(weighted * weighted, axis=1, keepdims=True) + EPSILON)
    flat = jnp.concatenate(
        [normed[g * kv + h : g * kv + h + 1, :] for h in range(kv) for g in range(group)], axis=1
    )
    read_ref[...] = (flat * read_gain_ref[...]).astype(BF16)

    @pl.loop(0, n)
    def _(i):
        k = step_pair(i, n)
        s = flip(me, k, n)

        @pl.when(k != 0)
        def _():
            block, sums = remote(i, s)
            sums.wait_send()
            block.wait_send()


def write_out(block_ref, sums_ref, read_ref, block_out, sums_out, read_out, sem):
    pairs = ((block_ref, block_out), (sums_ref, sums_out), (read_ref, read_out))
    copies = [pltpu.make_async_copy(a, b, sem.at[j]) for j, (a, b) in enumerate(pairs)]
    for copy in copies:
        copy.start()
    for copy in copies:
        copy.wait()


def local(
    n,
    prompt_block_input,
    key_projection_weight,
    value_projection_weight,
    forget_gate_weight,
    forget_gate_bias,
    forget_gate_scale,
    gate_spike_added,
    prior_key_value_cache,
    prior_cumulative_log_forget,
    decoded_token_query,
    decoded_token_key,
    decoded_token_value,
    decoded_log_gate,
    key_norm_gain,
    read_norm_gain,
):
    head_dim = key_norm_gain.shape[0]
    _, past, kv, width = prior_key_value_cache.shape
    _, span, model = prompt_block_input.shape
    group = decoded_token_query.shape[1] // (kv * head_dim)
    reps = max(group, -(-8 // kv))
    rows = reps * kv
    sub = 256
    chunk = 1024
    while past % chunk:
        chunk //= 2
    sub = min(sub, chunk)
    chunks = past // chunk
    block_rows = span * kv
    vmem = pl.BlockSpec(memory_space=pltpu.VMEM)
    hbm = pl.BlockSpec(memory_space=pl.ANY)
    new_cache, new_logc, read = pl.pallas_call(
        functools.partial(kernel, (n, span, kv, head_dim, group, reps, chunk, sub)),
        out_shape=(
            pltpu.VMEM((n, block_rows, width), BF16),
            pltpu.VMEM((kv, n * span), F32),
            pltpu.VMEM((1, group * kv * head_dim), BF16),
        ),
        in_specs=[hbm, hbm, hbm, vmem, vmem, vmem, vmem, hbm, hbm] + [vmem] * 6,
        out_specs=(vmem, vmem, vmem),
        scratch_shapes=[
            pltpu.VMEM((n, span, model), BF16),
            pltpu.VMEM((model, kv * head_dim), BF16),
            pltpu.VMEM((model, kv * head_dim), BF16),
            pltpu.VMEM((past * kv, width), BF16),
            pltpu.VMEM((kv, past), F32),
            pltpu.VMEM((block_rows, width), F32),
            pltpu.VMEM((n, block_rows, width), BF16),
            pltpu.VMEM((n, kv, span), F32),
            pltpu.VMEM((n, kv, span), F32),
            pltpu.VMEM((sub, sub * kv), BF16),
            pltpu.VMEM((n, rows, width), F32),
            pltpu.VMEM((n, rows, width), F32),
            pltpu.SemaphoreType.DMA((n,)),
            pltpu.SemaphoreType.DMA((2,)),
            pltpu.SemaphoreType.DMA((chunks,)),
            pltpu.SemaphoreType.DMA,
            pltpu.SemaphoreType.DMA((n,)),
            pltpu.SemaphoreType.DMA((n,)),
            pltpu.SemaphoreType.DMA((n,)),
            pltpu.SemaphoreType.DMA((n,)),
        ],
        compiler_params=pltpu.CompilerParams(
            collective_id=0, has_side_effects=True, vmem_limit_bytes=61 * 1024 * 1024
        ),
    )(
        prompt_block_input,
        key_projection_weight,
        value_projection_weight,
        forget_gate_weight,
        forget_gate_bias.reshape(1, -1),
        forget_gate_scale,
        gate_spike_added,
        prior_key_value_cache.reshape(past * kv, width),
        prior_cumulative_log_forget.reshape(kv, past),
        decoded_token_query,
        decoded_token_key,
        decoded_token_value,
        decoded_log_gate,
        key_norm_gain.reshape(1, -1),
        read_norm_gain.reshape(1, -1),
    )
    held = (new_cache, new_logc, read)
    new_cache, new_logc, read = pl.pallas_call(
        write_out,
        out_shape=tuple(jax.ShapeDtypeStruct(a.shape, a.dtype) for a in held),
        in_specs=[hbm] * 3,
        out_specs=(hbm, hbm, hbm),
        scratch_shapes=[pltpu.SemaphoreType.DMA((3,))],
        compiler_params=pltpu.CompilerParams(vmem_limit_bytes=1024 * 1024),
    )(*held)
    return (
        new_cache.reshape(1, n * span, kv, width),
        new_logc.reshape(1, kv, n * span),
        read,
    )


def solution(mesh):
    return jax.shard_map(
        functools.partial(local, mesh.shape["sp"]),
        mesh=mesh,
        in_specs=(
            P("gr", "sp", None),
            P(None, "tp"),
            P(None, "tp"),
            P("tp", None),
            P("tp"),
            P("gr", "tp", "sp"),
            P("gr", "tp", "sp"),
            P(("gr", "sp"), None, "tp", None),
            P(("gr", "sp"), "tp", None),
            P("gr", "tp"),
            P(("gr", "sp"), "tp"),
            P(("gr", "sp"), "tp"),
            P(("gr", "sp"), "tp"),
            P(),
            P("tp"),
        ),
        out_specs=(
            P(("gr", "sp"), None, "tp", None),
            P(("gr", "sp"), "tp", None),
            P(("gr", "sp"), "tp"),
        ),
        check_vma=False,
    )
```
